32 devices in a mesh: fs: 8 (over z, y), tp: 4 (over x, core).
Axes of the slice: x: 2, y: 2, z: 4, core: 2. Of those that a mesh axis runs over, the one named last changes fastest.
Arguments:
- hidden_in: bfloat16 [2048, 2048], P('fs'), may hold values from -6 to 6
- mix_gain: float32 [2048], replicated, may hold values from 0.1 to 1.9
- value_proj: float32 [2048, 512], P('fs', 'tp'), may hold values from -0.125 to 0.125
- gate_proj: float32 [2048, 512], P('fs', 'tp'), may hold values from -0.125 to 0.125
- out_proj: float32 [2048, 512], P('fs', 'tp'), may hold values from -0.25 to 0.25
- value_scale: float32 [512], P('tp'), may hold values from 0.3 to 3
- gate_scale: float32 [512], P('tp'), may hold values from 0.5 to 2
- out_scale: float32 [2048], P('fs'), may hold values from 0.5 to 2
- conv_kernel: bfloat16 [31, 512], P(None, 'tp'), may hold values from -1 to 1
- norm_gain: float32 [512], P('tp'), may hold values from 0.1 to 1.9
- norm_shift: float32 [512], P('tp'), may hold values from -3 to 3
- mlp_gain: float32 [2048], replicated, may hold values from 0.1 to 1.9
- mlp_gate: float32 [2048, 2816], P('fs', 'tp'), may hold values from -0.125 to 0.125
- mlp_up: float32 [2048, 2816], P('fs', 'tp'), may hold values from -0.125 to 0.125
- mlp_down: float32 [2048, 2816], P('fs', 'tp'), may hold values from -0.109375 to 0.109375
- mlp_gate_scale: float32 [2816], P('tp'), may hold values from 0.5 to 2
- mlp_up_scale: float32 [2816], P('tp'), may hold values from 0.5 to 2
- mlp_down_scale: float32 [2048], P('fs'), may hold values from 0.5 to 2
Outputs:
- layer_out: bfloat16 [2048, 2048], P('fs')
The draws below stay inside these ranges and needn't reach their ends.
All inputs are finite; a program needn't handle non-finite values.
Results may differ from the reference program's by a relative error of at most 0.019.
Values may be sent and summed in bfloat16 or wider, within the bound.
A program may use at most 64 MiB of HBM per device.

```python
import math
import jax
import jax.numpy as jnp
from jax import lax

D = 2048
CW = 512
FF = 2816
KW = 31
SEQ = 256
TOKENS = 2048
N_FS = 8
N_TP = 4


def draw_value_scale(key, part):
    column = jnp.arange(CW, dtype=jnp.float32) / CW
    base = jax.random.uniform(key, (CW,), jnp.float32, 0.0, 1.0)
    exponent = 0.5 * base + 0.5 * column
    return 0.3 * jnp.exp(jnp.log(10.0) * exponent)


def levels(rng, extent, split, smallest, top_value):
    level, own = 1.0, jax.random.fold_in(rng, 6)
    for axis_at, parts in split:
        heights = jnp.exp(jax.random.uniform(jax.random.fold_in(own, axis_at), (parts,), jnp.float32, smallest / len(split), top_value / len(split)))
        level = level * jnp.repeat(heights, extent[axis_at] // parts).reshape([-1 if axis == axis_at else 1 for axis in range(len(extent))])
    return level


def centred(own_key, extent, spread, reach, split=(), held_as=jnp.bfloat16):
    factor_of = levels(own_key, extent, split, -0.22, 0.18) if split else 1.0
    drawn = jax.random.normal(own_key, extent, jnp.float32) * spread * factor_of
    return jnp.minimum(jnp.maximum(drawn, -reach), reach).astype(held_as)


def setup_inputs(seed: int = 0) -> dict:
    streams_of = jax.random.split(jax.random.key(seed), 19)
    hidden_in = centred(streams_of[0], (TOKENS, D), 1.0, 6.0, ((0, 8),))
    mix_gain = jnp.clip(1.0 + 0.18 * jax.random.normal(streams_of[1], (D,), jnp.float32), 0.1, 1.9)
    value_proj = centred(streams_of[2], (D, CW), D ** -0.5, 0.125, ((0, 8), (1, 4)), jnp.float32)
    gate_proj = centred(streams_of[3], (D, CW), D ** -0.5, 0.125, ((0, 8), (1, 4)), jnp.float32)
    out_proj = centred(streams_of[4], (D, CW), CW ** -0.5, 0.25, ((0, 8), (1, 4)), jnp.float32)
    value_scale = draw_value_scale(jax.random.fold_in(streams_of[18], 71), 0)
    gate_scale = jnp.clip(jnp.exp(math.log(2.0) - 1.3862944 * jax.random.uniform(streams_of[6], (CW,), jnp.float32) ** levels(streams_of[6], (CW,), ((0, 4),), -0.2, 0.2)), 0.5, 2.0)
    out_scale = jnp.clip(jnp.exp(math.log(2.0) - 1.3862944 * jax.random.uniform(streams_of[7], (D,), jnp.float32) ** levels(streams_of[7], (D,), ((0, 8),), -0.2, 0.2)), 0.5, 2.0)
    conv_kernel = centred(streams_of[8], (KW, CW), KW ** -0.5, 1.0, ((1, 4),))
    norm_gain = jnp.clip(1.0 + 0.18 * jax.random.normal(streams_of[9], (CW,), jnp.float32), 0.1, 1.9)
    norm_shift = centred(streams_of[10], (CW,), 0.5, 3.0, ((0, 4),), jnp.float32)
    mlp_gain = jnp.clip(1.0 + 0.18 * jax.random.normal(streams_of[11], (D,), jnp.float32), 0.1, 1.9)
    mlp_gate = centred(streams_of[12], (D, FF), D ** -0.5, 0.125, ((0, 8), (1, 4)), jnp.float32)
    mlp_up = centred(streams_of[13], (D, FF), D ** -0.5, 0.125, ((0, 8), (1, 4)), jnp.float32)
    mlp_down = centred(streams_of[14], (D, FF), FF ** -0.5, 0.109375, ((0, 8), (1, 4)), jnp.float32)
    mlp_gate_scale = jnp.clip(jnp.exp(math.log(2.0) - 1.3862944 * jax.random.uniform(streams_of[15], (FF,), jnp.float32) ** levels(streams_of[15], (FF,), ((0, 4),), -0.2, 0.2)), 0.5, 2.0)
    mlp_up_scale = jnp.clip(jnp.exp(math.log(2.0) - 1.3862944 * jax.random.uniform(streams_of[16], (FF,), jnp.float32) ** levels(streams_of[16], (FF,), ((0, 4),), -0.2, 0.2)), 0.5, 2.0)
    mlp_down_scale = jnp.clip(jnp.exp(math.log(2.0) - 1.3862944 * jax.random.uniform(streams_of[17], (D,), jnp.float32) ** levels(streams_of[17], (D,), ((0, 8),), -0.2, 0.2)), 0.5, 2.0)
    return {"hidden_in": hidden_in, "mix_gain": mix_gain, "value_proj": value_proj, "gate_proj": gate_proj, "out_proj": out_proj, "value_scale": value_scale, "gate_scale": gate_scale, "out_scale": out_scale, "conv_kernel": conv_kernel, "norm_gain": norm_gain, "norm_shift": norm_shift, "mlp_gain": mlp_gain, "mlp_gate": mlp_gate, "mlp_up": mlp_up, "mlp_down": mlp_down, "mlp_gate_scale": mlp_gate_scale, "mlp_up_scale": mlp_up_scale, "mlp_down_scale": mlp_down_scale}


def row_norm(rows, gain):
    scale = lax.rsqrt(lax.optimization_barrier(jnp.mean(rows * rows, axis=-1, keepdims=True)) + 1e-06)
    return rows * scale * gain

def blocked_sum(act, weight_t, scale):
    width = act.shape[1] // N_TP
    total = jnp.zeros((act.shape[0], weight_t.shape[0]), jnp.float32)
    for block in range(N_TP):
        piece = act[:, block * width:(block + 1) * width]
        columns = weight_t[:, block * width:(block + 1) * width]
        term = lax.dot_general(piece, columns, (((1,), (1,)), ((), ())), preferred_element_type=jnp.float32) * scale
        rounded = lax.optimization_barrier(term.astype(jnp.bfloat16))
        total = total + rounded.astype(jnp.float32)
    return total

def one_sequence(rows_in, mix_gain, value_w, gate_w, out_w, value_scale, gate_scale, out_scale, conv_kernel, norm_gain, norm_shift, mlp_gain, mlp_gate_w, mlp_up_w, mlp_down_w, mlp_gate_scale, mlp_up_scale, mlp_down_scale):
    rows = rows_in.astype(jnp.float32)
    normed = row_norm(rows, mix_gain).astype(jnp.bfloat16)
    value_pre = jnp.dot(normed, value_w, preferred_element_type=jnp.float32) * value_scale
    gate_pre = jnp.dot(normed, gate_w, preferred_element_type=jnp.float32) * gate_scale
    glu = value_pre * jax.nn.sigmoid(gate_pre)
    padded = jnp.pad(glu, ((KW - 1, 0), (0, 0)))
    kernel = conv_kernel.astype(jnp.float32)
    conved = jnp.zeros_like(glu)
    for tap in range(KW):
        conved = conved + padded[tap:tap + SEQ] * kernel[tap]
    chan_mean = lax.optimization_barrier(jnp.mean(conved, axis=-1, keepdims=True))
    chan_var = lax.optimization_barrier(jnp.mean(conved * conved, axis=-1, keepdims=True)) - chan_mean * chan_mean
    act = jax.nn.silu((conved - chan_mean) * lax.rsqrt(chan_var + 1e-05) * norm_gain + norm_shift).astype(jnp.bfloat16)
    middle = (rows + blocked_sum(act, out_w, out_scale)).astype(jnp.bfloat16)
    middle_f = middle.astype(jnp.float32)
    normed_mlp = row_norm(middle_f, mlp_gain).astype(jnp.bfloat16)
    gate_mlp = jnp.dot(normed_mlp, mlp_gate_w, preferred_element_type=jnp.float32) * mlp_gate_scale
    up_mlp = jnp.dot(normed_mlp, mlp_up_w, preferred_element_type=jnp.float32) * mlp_up_scale
    hidden_act = (jax.nn.silu(gate_mlp) * up_mlp).astype(jnp.bfloat16)
    return (middle_f + blocked_sum(hidden_act, mlp_down_w, mlp_down_scale)).astype(jnp.bfloat16)

def reference(hidden_in, mix_gain, value_proj, gate_proj, out_proj, value_scale, gate_scale, out_scale, conv_kernel, norm_gain, norm_shift, mlp_gain, mlp_gate, mlp_up, mlp_down, mlp_gate_scale, mlp_up_scale, mlp_down_scale):
    weights = (value_proj.astype(jnp.bfloat16), gate_proj.astype(jnp.bfloat16), out_proj.astype(jnp.bfloat16), mlp_gate.astype(jnp.bfloat16), mlp_up.astype(jnp.bfloat16), mlp_down.astype(jnp.bfloat16))
    sequences = hidden_in.reshape(N_FS, SEQ, D)

    def apply(rows_in):
        return one_sequence(rows_in, mix_gain, weights[0], weights[1], weights[2], value_scale, gate_scale, out_scale, conv_kernel, norm_gain, norm_shift, mlp_gain, weights[3], weights[4], weights[5], mlp_gate_scale, mlp_up_scale, mlp_down_scale)
    return lax.map(apply, sequences).reshape(N_FS * SEQ, D)
```

```python
import functools

import jax
import jax.numpy as jnp
from jax import lax
from jax.experimental import pallas as pl
from jax.experimental.pallas import tpu as pltpu
from jax.sharding import PartitionSpec as P


def row_norm(rows, gain):
    scale = lax.rsqrt(jnp.mean(rows * rows, axis=-1, keepdims=True) + 1e-06)
    return rows * scale * gain


def contract_last(left, right):
    return lax.dot_general(
        left, right, (((1,), (1,)), ((), ())), preferred_element_type=jnp.float32
    )


def body(
    hidden_in,
    mix_gain,
    value_proj,
    gate_proj,
    out_proj,
    value_scale,
    gate_scale,
    out_scale,
    conv_kernel,
    norm_gain,
    norm_shift,
    mlp_gain,
    mlp_gate,
    mlp_up,
    mlp_down,
    mlp_gate_scale,
    mlp_up_scale,
    mlp_down_scale,
):
    out_full, down_full = (
        lax.all_gather(out_scale, "fs", axis=0, tiled=True),
        lax.all_gather(mlp_down_scale, "fs", axis=0, tiled=True),
    )
    value_w, gate_w, out_w = (
        lax.all_gather(value_proj.astype(jnp.bfloat16), "fs", axis=0, tiled=True),
        lax.all_gather(gate_proj.astype(jnp.bfloat16), "fs", axis=0, tiled=True),
        lax.all_gather(out_proj.astype(jnp.bfloat16), "fs", axis=0, tiled=True),
    )
    mlp_shards = (
        mlp_gate.astype(jnp.bfloat16),
        mlp_up.astype(jnp.bfloat16),
        mlp_down.astype(jnp.bfloat16),
    )
    rows = hidden_in.astype(jnp.float32)
    normed = row_norm(rows, mix_gain).astype(jnp.bfloat16)
    value_pre = jnp.dot(normed, value_w, preferred_element_type=jnp.float32) * value_scale
    gate_pre = jnp.dot(normed, gate_w, preferred_element_type=jnp.float32) * gate_scale
    glu = value_pre * jax.nn.sigmoid(gate_pre)
    seq_len = glu.shape[0]
    taps = conv_kernel.shape[0]
    padded = jnp.pad(glu, ((taps - 1, 0), (0, 0)))
    kernel = conv_kernel.astype(jnp.float32)
    conved = jnp.zeros_like(glu)
    for tap in range(taps):
        conved = conved + padded[tap : tap + seq_len] * kernel[tap]
    channels = conved.shape[1] * lax.axis_size("tp")
    sums, squares = lax.psum((jnp.sum(conved, axis=1), jnp.sum(conved * conved, axis=1)), "tp")
    chan_mean = (sums / channels)[:, None]
    chan_var = (squares / channels)[:, None] - chan_mean * chan_mean
    act = jax.nn.silu(
        (conved - chan_mean) * lax.rsqrt(chan_var + 1e-05) * norm_gain + norm_shift
    ).astype(jnp.bfloat16)
    conv_term = contract_last(act, out_w) * out_full
    middle_f = (
        (rows + lax.psum(conv_term.astype(jnp.bfloat16), "tp").astype(jnp.float32))
        .astype(jnp.bfloat16)
        .astype(jnp.float32)
    )
    normed_mlp = row_norm(middle_f, mlp_gain).astype(jnp.bfloat16)
    collected = (
        lax.all_gather(mlp_shards[0], "fs", axis=0, tiled=True),
        lax.all_gather(mlp_shards[1], "fs", axis=0, tiled=True),
        lax.all_gather(mlp_shards[2], "fs", axis=0, tiled=True),
    )
    gate_mlp = (
        jnp.dot(normed_mlp, collected[0], preferred_element_type=jnp.float32) * mlp_gate_scale
    )
    up_mlp = jnp.dot(normed_mlp, collected[1], preferred_element_type=jnp.float32) * mlp_up_scale
    hidden_act = (jax.nn.silu(gate_mlp) * up_mlp).astype(jnp.bfloat16)
    mlp_term = contract_last(hidden_act, collected[2]) * down_full
    return (middle_f + lax.psum(mlp_term.astype(jnp.bfloat16), "tp").astype(jnp.float32)).astype(
        jnp.bfloat16
    )


MESH = pl.DeviceIdType.MESH
LANES = 128
Y = 2
CORES = 2


def nearest_order(z, extent):
    picks = []
    for k in range(extent):
        pick = jnp.int32(0)
        for at in range(extent):
            order = sorted(range(extent), key=lambda v: (abs(v - at), v))
            pick = jnp.where(z == at, order[k], pick)
        picks.append(pick)
    return picks


def layer_kernel(
    Z,
    hidden, mix_gain, value_p, gate_p, out_p, value_s, gate_s, out_s, taps_ref,
    norm_gain, norm_shift, mlp_gain, mgate, mup, mdown, mgate_s, mup_s, mdown_s,
    result,
    vg, ow, gu, dn, normed, pad, mid, acc, hid, stat_out, stat_in, stat_t,
    core_out, core_in, x_out, x_in,
    g_send, g_recv, s_send, s_recv, c_send, c_recv, x_send, x_recv, f_send, f_recv,
):
    f32, bf16 = jnp.float32, jnp.bfloat16
    fs, tp = lax.axis_index("fs"), lax.axis_index("tp")
    z, y = fs // Y, lax.rem(fs, Y)
    x, core = tp // CORES, lax.rem(tp, CORES)
    yo = 1 - y
    me = (fs, tp)
    up, down = (fs + Y, tp), (fs - Y, tp)
    across = (z * Y + yo, tp)
    core_peer = (fs, x * CORES + 1 - core)
    x_peer = (fs, (1 - x) * CORES + core)
    diag_peer = (fs, (1 - x) * CORES + 1 - core)
    has_up, has_down = z < Z - 1, z > 0

    rows, width = hidden.shape
    nblk = Z * Y
    blk = width // nblk
    ch = value_p.shape[1]
    hu = mgate.shape[1]

    vg[fs, :, :ch] = value_p[...].astype(bf16)
    vg[fs, :, ch:] = gate_p[...].astype(bf16)
    scale_col = jnp.broadcast_to(out_s[...], (LANES, blk)).T
    ow[fs] = (out_p[...].astype(bf16).astype(f32) * scale_col[:, :1]).astype(bf16)

    barrier = pltpu.get_barrier_semaphore()

    def greet(peer):
        pl.semaphore_signal(barrier, inc=1, device_id=peer, device_id_type=MESH)

    for peer in (across, core_peer, x_peer, diag_peer):
        greet(peer)

    @pl.when(has_up)
    def _():
        greet(up)

    @pl.when(has_down)
    def _():
        greet(down)

    pl.semaphore_wait(barrier, 4 + has_up.astype(jnp.int32) + has_down.astype(jnp.int32))

    half = blk // 2
    quarter = blk // 4
    pieces = [(vg, None), (ow, None)]
    pieces += [(gu, (r * quarter, quarter)) for r in range(4)]
    pieces += [(dn, (r * quarter, quarter)) for r in range(2)]
    crossed = (3,)

    def slot(p, at):
        ref, cut = pieces[p]
        return ref.at[at] if cut is None else ref.at[at, pl.ds(*cut)]

    def copy(p, at, peer, way):
        return pltpu.make_async_remote_copy(
            src_ref=slot(p, at), dst_ref=slot(p, at),
            send_sem=g_send.at[p, at, way], recv_sem=g_recv.at[p, at],
            device_id=peer, device_id_type=MESH,
        )

    sent = []

    def start(p, at, peer, way, cond=None):
        if cond is None:
            copy(p, at, peer, way).start()
        else:
            @pl.when(cond)
            def _():
                copy(p, at, peer, way).start()
        sent.append((p, at, peer, way, cond))

    def own(p):
        start(p, fs, up, 0, has_up)
        start(p, fs, down, 1, has_down)
        start(p, fs, across, 2)

    def arrived(p, at):
        copy(p, at, across, 2).wait_recv()

    def own_crossed(p):
        at = z * Y + yo
        arrived(p, at)
        start(p, at, up, 0, has_up)
        start(p, at, down, 1, has_down)

    def relay(p, s):
        lanes = (y, yo) if p in crossed else (y,)
        for lane in lanes:
            below, above = (z - s) * Y + lane, (z + s) * Y + lane
            ok_b, ok_a = z - s >= 0, z + s < Z

            @pl.when(ok_b)
            def _(below=below):
                arrived(p, below)

            start(p, below, up, 0, jnp.logical_and(ok_b, has_up))
            if p not in crossed:
                start(p, below, across, 2, ok_b)

            @pl.when(ok_a)
            def _(above=above):
                arrived(p, above)

            start(p, above, down, 1, jnp.logical_and(ok_a, has_down))
            if p not in crossed:
                start(p, above, across, 2, ok_a)

    def finish(p, zz=None):
        if p not in crossed:
            for at in range(Z) if zz is None else (zz,):
                arrived(p, at * Y + yo)

    def wave(t):
        q0, count = 2, len(pieces) - 2
        if t < count:
            own(q0 + t)
        if 0 <= t - 1 < count:
            if q0 + t - 1 in crossed:
                own_crossed(q0 + t - 1)
        for s in range(1, Z):
            if 0 <= t - s < count:
                relay(q0 + t - s, s)

    own(0)
    own(1)

    gu[fs, :, :hu] = mgate[...].astype(bf16)
    gu[fs, :, hu:] = mup[...].astype(bf16)
    scale_col = jnp.broadcast_to(mdown_s[...], (LANES, blk)).T
    folded = (mdown[...].astype(bf16).astype(f32) * scale_col[:, :1]).astype(bf16)
    dn[fs, :, :hu] = folded[:half]
    dn[fs, :, hu:] = folded[half:]

    relay(0, 1)
    relay(1, 1)

    h = hidden[...].astype(f32)
    norm = lax.rsqrt(jnp.mean(h * h, axis=-1, keepdims=True) + 1e-06)
    for b in range(nblk):
        cols = slice(b * blk, (b + 1) * blk)
        normed[b] = (hidden[:, cols].astype(f32) * norm * mix_gain[:, cols]).astype(bf16)

    for s in range(2, Z):
        relay(0, s)
        relay(1, s)
    wave(0)
    finish(0)

    pre = jnp.zeros((rows, 2 * ch), f32)
    for b in range(nblk):
        pre += jnp.dot(normed[b], vg[b], preferred_element_type=f32)
    glu = pre[:, :ch] * value_s[...] * jax.nn.sigmoid(pre[:, ch:] * gate_s[...])
    ntaps = taps_ref.shape[0]
    lead = pad.shape[0] - rows
    pad[pl.ds(0, lead)] = jnp.zeros((lead, ch), f32)
    pad[pl.ds(lead, rows)] = glu
    taps = taps_ref[...].astype(f32)
    conved = jnp.zeros((rows, ch), f32)
    for j in range(ntaps):
        conved += pad[pl.ds(lead - ntaps + 1 + j, rows)] * taps[j : j + 1]
    lane = lax.broadcasted_iota(jnp.int32, (rows, LANES), 1)
    packed = jnp.where(
        lane == 0,
        jnp.sum(conved, axis=1, keepdims=True),
        jnp.sum(conved * conved, axis=1, keepdims=True),
    )
    stat_t[...] = packed.T
    stat_out[...] = stat_t[:8]

    def stat_copy(k, peer):
        return pltpu.make_async_remote_copy(
            src_ref=stat_out, dst_ref=stat_in.at[k],
            send_sem=s_send.at[k], recv_sem=s_recv.at[k],
            device_id=peer, device_id_type=MESH,
        )

    stats = [stat_copy(k, p) for k, p in enumerate((core_peer, x_peer, diag_peer))]
    for c in stats:
        c.start()
    wave(1)
    for c in stats:
        c.wait()
    stat_t[pl.ds(0, 8)] = stat_out[...] + stat_in[0] + stat_in[1] + stat_in[2]
    columns = stat_t[...].T
    channels = ch * CORES * 2
    mean = columns[:, 0:1] / channels
    var = columns[:, 1:2] / channels - mean * mean
    a = (conved - mean) * lax.rsqrt(var + 1e-05) * norm_gain[...] + norm_shift[...]
    act = (a * jax.nn.sigmoid(a)).astype(bf16)
    finish(1)

    order = nearest_order(z, Z)
    mine, theirs = lax.rem(y + core, Y), lax.rem(y + 1 - core, Y)

    def core_copy(u, k):
        return pltpu.make_async_remote_copy(
            src_ref=core_out.at[u, k], dst_ref=core_in.at[u, k],
            send_sem=c_send.at[u, k], recv_sem=c_recv.at[u, k],
            device_id=core_peer, device_id_type=MESH,
        )

    def x_copy(u, k):
        return pltpu.make_async_remote_copy(
            src_ref=x_out.at[u, k], dst_ref=x_in.at[u, k],
            send_sem=x_send.at[u, k], recv_sem=x_recv.at[u, k],
            device_id=x_peer, device_id_type=MESH,
        )

    def final_copy(u, ref, at):
        return pltpu.make_async_remote_copy(
            src_ref=ref.at[at], dst_ref=ref.at[at],
            send_sem=f_send.at[u, at], recv_sem=f_recv.at[u, at],
            device_id=core_peer, device_id_type=MESH,
        )

    def conv_term(b):
        return lax.dot_general(act, ow[b], (((1,), (1,)), ((), ())), preferred_element_type=f32)

    for k in range(Z):
        core_out[0, k] = conv_term(order[k] * Y + theirs).astype(bf16)
        core_copy(0, k).start()
    wave(2)
    for k in range(Z):
        term = conv_term(order[k] * Y + mine)
        core_copy(0, k).wait_recv()
        x_out[0, k] = (term + core_in[0, k].astype(f32)).astype(bf16)
        x_copy(0, k).start()
    wave(3)
    for k in range(Z):
        b = order[k] * Y + mine
        x_copy(0, k).wait_recv()
        cols = pl.ds(pl.multiple_of(b * blk, blk), blk)
        total = x_out[0, k].astype(f32) + x_in[0, k].astype(f32)
        mid[b] = (hidden[:, cols].astype(f32) + total).astype(bf16)
        final_copy(0, mid, b).start()
    wave(4)
    for k in range(Z):
        final_copy(0, mid, order[k] * Y + theirs).wait_recv()

    total = jnp.zeros((rows, 1), f32)
    for b in range(nblk):
        m = mid[b].astype(f32)
        total += jnp.sum(m * m, axis=-1, keepdims=True)
    norm = lax.rsqrt(total / width + 1e-06)
    for b in range(nblk):
        cols = slice(b * blk, (b + 1) * blk)
        normed[b] = (mid[b].astype(f32) * norm * mlp_gain[:, cols]).astype(bf16)
    for t in range(5, len(pieces) - 2 + Z - 1):
        wave(t)

    for p in range(2, 6):
        finish(p)
    acc[...] = jnp.dot(normed[0], gu[0], preferred_element_type=f32)

    def step(b, carry):
        acc[...] += jnp.dot(normed[b], gu[b], preferred_element_type=f32)
        return carry

    lax.fori_loop(1, nblk, step, 0)
    gate = acc[:, :hu] * mgate_s[...]
    up_v = acc[:, hu:] * mup_s[...]
    act2 = (gate * jax.nn.sigmoid(gate) * up_v).astype(bf16)
    zero = jnp.zeros_like(act2)
    hid[0, :, :hu] = act2
    hid[0, :, hu:] = zero
    hid[1, :, :hu] = zero
    hid[1, :, hu:] = act2

    dims = (((1,), (1,)), ((), ()))

    def mlp_term(b):
        return [
            lax.dot_general(hid[i], dn[b], dims, preferred_element_type=f32) for i in range(2)
        ]

    def send_theirs(k):
        for i, t in enumerate(mlp_term(order[k] * Y + theirs)):
            core_out[1, k, :, i * half : (i + 1) * half] = t.astype(bf16)
        core_copy(1, k).start()

    def send_mine(k):
        terms = mlp_term(order[k] * Y + mine)
        core_copy(1, k).wait_recv()
        for i, t in enumerate(terms):
            cols = slice(i * half, (i + 1) * half)
            x_out[1, k, :, cols] = (t + core_in[1, k, :, cols].astype(f32)).astype(bf16)
        x_copy(1, k).start()

    def send_final(k):
        b = order[k] * Y + mine
        x_copy(1, k).wait_recv()
        total = x_out[1, k].astype(f32) + x_in[1, k].astype(f32)
        result[b] = (mid[b].astype(f32) + total).astype(bf16)
        final_copy(1, result, b).start()

    for k in range(Z):
        finish(6, order[k])
        finish(7, order[k])
        send_theirs(k)
        send_mine(k)
        if k:
            send_final(k - 1)
    send_final(Z - 1)
    for k in range(Z):
        final_copy(1, result, order[k] * Y + theirs).wait_recv()

    for p, at, peer, way, cond in sent:
        if cond is None:
            copy(p, at, peer, way).wait_send()
        else:
            @pl.when(cond)
            def _(p=p, at=at, peer=peer, way=way):
                copy(p, at, peer, way).wait_send()
    for u, ref in ((0, mid), (1, result)):
        for k in range(Z):
            core_copy(u, k).wait_send()
            x_copy(u, k).wait_send()
            final_copy(u, ref, order[k] * Y + mine).wait_send()


def kernel_body(*args):
    n_fs = lax.axis_size("fs")
    Z = n_fs // Y
    hidden, value_p, taps, mgate = args[0], args[2], args[8], args[12]
    rows, width = hidden.shape
    blk, ch, hu = width // n_fs, value_p.shape[1], mgate.shape[1]
    args = [a.reshape(1, -1) if a.ndim == 1 else a for a in args]
    lead = -(-(taps.shape[0] - 1) // 8) * 8
    bf16, f32 = jnp.bfloat16, jnp.float32
    dma = pltpu.SemaphoreType.DMA
    n_pieces = 8
    out = pl.pallas_call(
        functools.partial(layer_kernel, Z),
        out_shape=jax.ShapeDtypeStruct((n_fs, rows, blk), bf16),
        in_specs=[pl.BlockSpec(memory_space=pltpu.VMEM)] * len(args),
        out_specs=pl.BlockSpec(memory_space=pltpu.VMEM),
        scratch_shapes=[
            pltpu.VMEM((n_fs, blk, 2 * ch), bf16),
            pltpu.VMEM((n_fs, blk, ch), bf16),
            pltpu.VMEM((n_fs, blk, 2 * hu), bf16),
            pltpu.VMEM((n_fs, blk // 2, 2 * hu), bf16),
            pltpu.VMEM((n_fs, rows, blk), bf16),
            pltpu.VMEM((lead + rows, ch), f32),
            pltpu.VMEM((n_fs, rows, blk), bf16),
            pltpu.VMEM((rows, 2 * hu), f32),
            pltpu.VMEM((2, rows, 2 * hu), bf16),
            pltpu.VMEM((8, rows), f32),
            pltpu.VMEM((3, 8, rows), f32),
            pltpu.VMEM((LANES, rows), f32),
            pltpu.VMEM((2, Z, rows, blk), bf16),
            pltpu.VMEM((2, Z, rows, blk), bf16),
            pltpu.VMEM((2, Z, rows, blk), bf16),
            pltpu.VMEM((2, Z, rows, blk), bf16),
            dma((n_pieces, n_fs, 3)),
            dma((n_pieces, n_fs)),
            dma((3,)),
            dma((3,)),
            dma((2, Z)),
            dma((2, Z)),
            dma((2, Z)),
            dma((2, Z)),
            dma((2, n_fs)),
            dma((2, n_fs)),
        ],
        compiler_params=pltpu.CompilerParams(
            collective_id=0, has_side_effects=True, vmem_limit_bytes=56 * 1024 * 1024
        ),
    )(*args)
    return out.transpose(1, 0, 2).reshape(rows, width)


def fits(mesh, args):
    n_fs, n_tp = mesh.shape["fs"], mesh.shape["tp"]
    ch, hu = args[2].shape[1] // n_tp, args[12].shape[1] // n_tp
    blk = args[0].shape[1] // n_fs
    return (
        n_fs % Y == 0
        and n_tp == 2 * CORES
        and ch % LANES == 0
        and (2 * hu) % LANES == 0
        and blk % (2 * LANES) == 0
        and n_fs <= 8
    )


SPECS = (
    P("fs", None), P(), P("fs", "tp"), P("fs", "tp"), P("fs", "tp"), P("tp"), P("tp"),
    P("fs"), P(None, "tp"), P("tp"), P("tp"), P(), P("fs", "tp"), P("fs", "tp"),
    P("fs", "tp"), P("tp"), P("tp"), P("fs"),
)


def solution(mesh):
    def run(*args):
        return jax.shard_map(
            kernel_body if fits(mesh, args) else body,
            mesh=mesh, in_specs=SPECS, out_specs=P("fs", None), check_vma=False,
        )(*args)

    return run
```

```python
import functools

import jax
import jax.numpy as jnp
from jax import lax
from jax.experimental import pallas as pl
from jax.experimental.pallas import tpu as pltpu
from jax.sharding import PartitionSpec as P


def row_norm(rows, gain):
    scale = lax.rsqrt(jnp.mean(rows * rows, axis=-1, keepdims=True) + 1e-06)
    return rows * scale * gain


def contract_last(left, right):
    return lax.dot_general(
        left, right, (((1,), (1,)), ((), ())), preferred_element_type=jnp.float32
    )


def body(
    hidden_in,
    mix_gain,
    value_proj,
    gate_proj,
    out_proj,
    value_scale,
    gate_scale,
    out_scale,
    conv_kernel,
    norm_gain,
    norm_shift,
    mlp_gain,
    mlp_gate,
    mlp_up,
    mlp_down,
    mlp_gate_scale,
    mlp_up_scale,
    mlp_down_scale,
):
    out_full, down_full = (
        lax.all_gather(out_scale, "fs", axis=0, tiled=True),
        lax.all_gather(mlp_down_scale, "fs", axis=0, tiled=True),
    )
    value_w, gate_w, out_w = (
        lax.all_gather(value_proj.astype(jnp.bfloat16), "fs", axis=0, tiled=True),
        lax.all_gather(gate_proj.astype(jnp.bfloat16), "fs", axis=0, tiled=True),
        lax.all_gather(out_proj.astype(jnp.bfloat16), "fs", axis=0, tiled=True),
    )
    mlp_shards = (
        mlp_gate.astype(jnp.bfloat16),
        mlp_up.astype(jnp.bfloat16),
        mlp_down.astype(jnp.bfloat16),
    )
    rows = hidden_in.astype(jnp.float32)
    normed = row_norm(rows, mix_gain).astype(jnp.bfloat16)
    value_pre = jnp.dot(normed, value_w, preferred_element_type=jnp.float32) * value_scale
    gate_pre = jnp.dot(normed, gate_w, preferred_element_type=jnp.float32) * gate_scale
    glu = value_pre * jax.nn.sigmoid(gate_pre)
    seq_len = glu.shape[0]
    taps = conv_kernel.shape[0]
    padded = jnp.pad(glu, ((taps - 1, 0), (0, 0)))
    kernel = conv_kernel.astype(jnp.float32)
    conved = jnp.zeros_like(glu)
    for tap in range(taps):
        conved = conved + padded[tap : tap + seq_len] * kernel[tap]
    channels = conved.shape[1] * lax.axis_size("tp")
    sums, squares = lax.psum((jnp.sum(conved, axis=1), jnp.sum(conved * conved, axis=1)), "tp")
    chan_mean = (sums / channels)[:, None]
    chan_var = (squares / channels)[:, None] - chan_mean * chan_mean
    act = jax.nn.silu(
        (conved - chan_mean) * lax.rsqrt(chan_var + 1e-05) * norm_gain + norm_shift
    ).astype(jnp.bfloat16)
    conv_term = contract_last(act, out_w) * out_full
    middle_f = (
        (rows + lax.psum(conv_term.astype(jnp.bfloat16), "tp").astype(jnp.float32))
        .astype(jnp.bfloat16)
        .astype(jnp.float32)
    )
    normed_mlp = row_norm(middle_f, mlp_gain).astype(jnp.bfloat16)
    collected = (
        lax.all_gather(mlp_shards[0], "fs", axis=0, tiled=True),
        lax.all_gather(mlp_shards[1], "fs", axis=0, tiled=True),
        lax.all_gather(mlp_shards[2], "fs", axis=0, tiled=True),
    )
    gate_mlp = (
        jnp.dot(normed_mlp, collected[0], preferred_element_type=jnp.float32) * mlp_gate_scale
    )
    up_mlp = jnp.dot(normed_mlp, collected[1], preferred_element_type=jnp.float32) * mlp_up_scale
    hidden_act = (jax.nn.silu(gate_mlp) * up_mlp).astype(jnp.bfloat16)
    mlp_term = contract_last(hidden_act, collected[2]) * down_full
    return (middle_f + lax.psum(mlp_term.astype(jnp.bfloat16), "tp").astype(jnp.float32)).astype(
        jnp.bfloat16
    )


MESH = pl.DeviceIdType.MESH
LANES = 128
Y = 2
CORES = 2
ROW = 1024
AHEAD_Y = 3
AHEAD_Z = 2


def nearest_order(z, extent):
    picks = []
    for k in range(extent):
        pick = jnp.int32(0)
        for at in range(extent):
            order = sorted(range(extent), key=lambda v: (abs(v - at), v))
            pick = jnp.where(z == at, order[k], pick)
        picks.append(pick)
    return picks


def layer_kernel(
    Z,
    hidden_hbm, mix_gain, value_p, gate_p, out_p, value_s, gate_s, out_s, taps_ref,
    norm_gain, norm_shift, mlp_gain, mgate_hbm, mup_hbm, mdown_hbm, mid_s, mdown_s,
    result_hbm,
    hidden, mgate, mup, mdown, result,
    vg, ow, gu, dn, normed, pad, mid, acc, acc_up, stat_out, stat_in, stat_t,
    core_out, core_in, x_out, x_in,
    g_send, g_recv, s_send, s_recv, c_send, c_recv, x_send, x_recv, f_send, f_recv,
    l_sem, o_sem,
):
    f32, bf16 = jnp.float32, jnp.bfloat16
    fs, tp = lax.axis_index("fs"), lax.axis_index("tp")
    z, y = fs // Y, lax.rem(fs, Y)
    x, core = tp // CORES, lax.rem(tp, CORES)
    yo = 1 - y
    me = (fs, tp)
    up, down = (fs + Y, tp), (fs - Y, tp)
    across = (z * Y + yo, tp)
    core_peer = (fs, x * CORES + 1 - core)
    x_peer = (fs, (1 - x) * CORES + core)
    diag_peer = (fs, (1 - x) * CORES + 1 - core)
    has_up, has_down = z < Z - 1, z > 0

    rows, width = hidden.shape
    nblk = Z * Y
    blk = width // nblk
    ch = value_p.shape[1]
    hu = mgate.shape[0]
    fetches = [
        pltpu.make_async_copy(src, dst, l_sem.at[i])
        for i, (src, dst) in enumerate(
            ((hidden_hbm, hidden), (mgate_hbm, mgate), (mup_hbm, mup), (mdown_hbm, mdown))
        )
    ]
    for f in fetches:
        f.start()

    vg[fs, :, :ch] = value_p[...].astype(bf16)
    vg[fs, :, ch:] = gate_p[...].astype(bf16)
    scale_col = jnp.broadcast_to(out_s[...], (LANES, blk)).T
    ow[fs] = (out_p[...].astype(bf16).astype(f32) * scale_col[:, :1]).astype(bf16)

    barrier = pltpu.get_barrier_semaphore()

    def greet(peer):
        pl.semaphore_signal(barrier, inc=1, device_id=peer, device_id_type=MESH)

    for peer in (across, core_peer, x_peer, diag_peer):
        greet(peer)

    @pl.when(has_up)
    def _():
        greet(up)

    @pl.when(has_down)
    def _():
        greet(down)

    pl.semaphore_wait(barrier, 4 + has_up.astype(jnp.int32) + has_down.astype(jnp.int32))

    quarter = hu // 2
    pieces = [(vg, None), (ow, None)]
    pieces += [(gu, (r * quarter, quarter)) for r in range(4)]
    pieces += [(dn, (r * quarter, quarter)) for r in range(2)]
    crossed = (3,)

    def slot(p, at):
        ref, cut = pieces[p]
        return ref.at[at] if cut is None else ref.at[at, pl.ds(*cut)]

    def copy(p, at, peer, way):
        return pltpu.make_async_remote_copy(
            src_ref=slot(p, at), dst_ref=slot(p, at),
            send_sem=g_send.at[p, at, way], recv_sem=g_recv.at[p, at],
            device_id=peer, device_id_type=MESH,
        )

    sent = []

    def start(p, at, peer, way, cond=None):
        if cond is None:
            copy(p, at, peer, way).start()
        else:
            @pl.when(cond)
            def _():
                copy(p, at, peer, way).start()
        sent.append((p, at, peer, way, cond))

    def own_z(p):
        start(p, fs, up, 0, has_up)
        start(p, fs, down, 1, has_down)

    def own_y(p):
        start(p, fs, across, 2)

    def own(p):
        own_y(p)
        own_z(p)

    def arrived(p, at):
        copy(p, at, across, 2).wait_recv()

    def own_crossed(p):
        at = z * Y + yo
        arrived(p, at)
        start(p, at, up, 0, has_up)
        start(p, at, down, 1, has_down)

    def relay(p, s):
        lanes = (y, yo) if p in crossed else (y,)
        for lane in lanes:
            below, above = (z - s) * Y + lane, (z + s) * Y + lane
            ok_b, ok_a = z - s >= 0, z + s < Z

            @pl.when(ok_b)
            def _(below=below):
                arrived(p, below)

            start(p, below, up, 0, jnp.logical_and(ok_b, has_up))
            if p not in crossed:
                start(p, below, across, 2, ok_b)

            @pl.when(ok_a)
            def _(above=above):
                arrived(p, above)

            start(p, above, down, 1, jnp.logical_and(ok_a, has_down))
            if p not in crossed:
                start(p, above, across, 2, ok_a)

    def finish(p, zz=None):
        if p not in crossed:
            for at in range(Z) if zz is None else (zz,):
                arrived(p, at * Y + yo)

    def wave(t):
        q0, count = 2, len(pieces) - 2
        for q in range(AHEAD_Y + 1) if t == 0 else (t + AHEAD_Y,):
            if q < count:
                own_y(q0 + q)
        for q in range(AHEAD_Z + 1) if t == 0 else (t + AHEAD_Z,):
            if q < count:
                own_z(q0 + q)
        if 0 <= t - 1 < count:
            if q0 + t - 1 in crossed:
                own_crossed(q0 + t - 1)
        for s in range(1, Z):
            if 0 <= t - s < count:
                relay(q0 + t - s, s)

    own(0)
    own(1)

    for f in fetches:
        f.wait()
    gu[fs, :hu] = mgate[...].astype(bf16)
    gu[fs, hu:] = mup[...].astype(bf16)
    dn[fs] = (mdown[...].astype(bf16).astype(f32) * mdown_s[...]).astype(bf16)

    relay(0, 1)
    relay(1, 1)

    h = hidden[...].astype(f32)
    norm = lax.rsqrt(jnp.mean(h * h, axis=-1, keepdims=True) + 1e-06)
    for b in range(nblk):
        cols = slice(b * blk, (b + 1) * blk)
        normed[b] = (hidden[:, cols].astype(f32) * norm * mix_gain[:, cols]).astype(bf16)

    for s in range(2, Z):
        relay(0, s)
        relay(1, s)
    wave(0)
    finish(0)

    pre = jnp.zeros((rows, 2 * ch), f32)
    for b in range(nblk):
        pre += jnp.dot(normed[b], vg[b], preferred_element_type=f32)
    glu = pre[:, :ch] * value_s[...] * jax.nn.sigmoid(pre[:, ch:] * gate_s[...])
    ntaps = taps_ref.shape[0]
    lead = pad.shape[0] - rows
    pad[pl.ds(0, lead)] = jnp.zeros((lead, ch), f32)
    pad[pl.ds(lead, rows)] = glu
    taps = taps_ref[...].astype(f32)
    conved = jnp.zeros((rows, ch), f32)
    for j in range(ntaps):
        conved += pad[pl.ds(lead - ntaps + 1 + j, rows)] * taps[j : j + 1]
    lane = lax.broadcasted_iota(jnp.int32, (rows, LANES), 1)
    packed = jnp.where(
        lane == 0,
        jnp.sum(conved, axis=1, keepdims=True),
        jnp.sum(conved * conved, axis=1, keepdims=True),
    )
    stat_t[...] = packed.T
    stat_out[...] = stat_t[:8]

    def stat_copy(k, peer):
        return pltpu.make_async_remote_copy(
            src_ref=stat_out, dst_ref=stat_in.at[k],
            send_sem=s_send.at[k], recv_sem=s_recv.at[k],
            device_id=peer, device_id_type=MESH,
        )

    stats = [stat_copy(k, p) for k, p in enumerate((core_peer, x_peer, diag_peer))]
    for c in stats:
        c.start()
    wave(1)
    for c in stats:
        c.wait()
    stat_t[pl.ds(0, 8)] = stat_out[...] + stat_in[0] + stat_in[1] + stat_in[2]
    columns = stat_t[...].T
    channels = ch * CORES * 2
    mean = columns[:, 0:1] / channels
    var = columns[:, 1:2] / channels - mean * mean
    a = (conved - mean) * lax.rsqrt(var + 1e-05) * norm_gain[...] + norm_shift[...]
    act = (a * jax.nn.sigmoid(a)).astype(bf16)
    finish(1)

    order = nearest_order(z, Z)
    mine, theirs = lax.rem(y + core, Y), lax.rem(y + 1 - core, Y)

    def core_copy(u, k):
        return pltpu.make_async_remote_copy(
            src_ref=core_out.at[u, k], dst_ref=core_in.at[u, k],
            send_sem=c_send.at[u, k], recv_sem=c_recv.at[u, k],
            device_id=core_peer, device_id_type=MESH,
        )

    def x_copy(u, k):
        return pltpu.make_async_remote_copy(
            src_ref=x_out.at[u, k], dst_ref=x_in.at[u, k],
            send_sem=x_send.at[u, k], recv_sem=x_recv.at[u, k],
            device_id=x_peer, device_id_type=MESH,
        )

    def final_copy(u, ref, at):
        return pltpu.make_async_remote_copy(
            src_ref=ref.at[at], dst_ref=ref.at[at],
            send_sem=f_send.at[u, at], recv_sem=f_recv.at[u, at],
            device_id=core_peer, device_id_type=MESH,
        )

    def conv_term(b):
        return lax.dot_general(act, ow[b], (((1,), (1,)), ((), ())), preferred_element_type=f32)

    for k in range(Z):
        core_out[0, k] = conv_term(order[k] * Y + theirs).astype(bf16)
        core_copy(0, k).start()
    wave(2)
    for k in range(Z):
        term = conv_term(order[k] * Y + mine)
        core_copy(0, k).wait_recv()
        x_out[0, k] = (term + core_in[0, k].astype(f32)).astype(bf16)
        x_copy(0, k).start()
    wave(3)
    for k in range(Z):
        b = order[k] * Y + mine
        x_copy(0, k).wait_recv()
        cols = pl.ds(pl.multiple_of(b * blk, blk), blk)
        total = x_out[0, k].astype(f32) + x_in[0, k].astype(f32)
        mid[b] = (hidden[:, cols].astype(f32) + total).astype(bf16)
        final_copy(0, mid, b).start()
    wave(4)
    for k in range(Z):
        final_copy(0, mid, order[k] * Y + theirs).wait_recv()

    total = jnp.zeros((rows, 1), f32)
    for b in range(nblk):
        m = mid[b].astype(f32)
        total += jnp.sum(m * m, axis=-1, keepdims=True)
    norm = lax.rsqrt(total / width + 1e-06)
    for b in range(nblk):
        cols = slice(b * blk, (b + 1) * blk)
        normed[b] = (mid[b].astype(f32) * norm * mlp_gain[:, cols]).astype(bf16)
    for t in range(5, len(pieces) - 2 + Z - 1):
        wave(t)

    for p in range(2, 6):
        finish(p)
    dims = (((1,), (1,)), ((), ()))

    def gate_up(b):
        return (
            lax.dot_general(normed[b], gu[b, :hu], dims, preferred_element_type=f32),
            lax.dot_general(normed[b], gu[b, hu:], dims, preferred_element_type=f32),
        )

    acc[...], acc_up[...] = gate_up(0)

    def step(b, carry):
        g, u = gate_up(b)
        acc[...] += g
        acc_up[...] += u
        return carry

    lax.fori_loop(1, nblk, step, 0)
    gate = acc[...] * mid_s[:, :hu]
    second = mid_s.shape[1] // 2
    up_v = acc_up[...] * mid_s[:, second : second + hu]
    act2 = (gate * jax.nn.sigmoid(gate) * up_v).astype(bf16)

    def mlp_term(b):
        return jnp.dot(act2, dn[b], preferred_element_type=f32)

    def send_theirs(k):
        core_out[1, k] = mlp_term(order[k] * Y + theirs).astype(bf16)
        core_copy(1, k).start()

    def send_mine(k):
        term = mlp_term(order[k] * Y + mine)
        core_copy(1, k).wait_recv()
        x_out[1, k] = (term + core_in[1, k].astype(f32)).astype(bf16)
        x_copy(1, k).start()

    def send_final(k):
        b = order[k] * Y + mine
        x_copy(1, k).wait_recv()
        total = x_out[1, k].astype(f32) + x_in[1, k].astype(f32)
        result[b] = (mid[b].astype(f32) + total).astype(bf16)
        final_copy(1, result, b).start()
        out_copy(b).start()

    def out_copy(b):
        cols = pl.ds(pl.multiple_of(b * blk, blk), blk)
        return pltpu.make_async_copy(result.at[b], result_hbm.at[:, cols], o_sem.at[b])

    for k in range(Z):
        finish(6, order[k])
        finish(7, order[k])
        send_theirs(k)
        send_mine(k)
        if k:
            send_final(k - 1)
    send_final(Z - 1)
    for k in range(Z):
        b = order[k] * Y + theirs
        final_copy(1, result, b).wait_recv()
        out_copy(b).start()
    for b in range(nblk):
        out_copy(b).wait()

    for p, at, peer, way, cond in sent:
        if cond is None:
            copy(p, at, peer, way).wait_send()
        else:
            @pl.when(cond)
            def _(p=p, at=at, peer=peer, way=way):
                copy(p, at, peer, way).wait_send()
    for u, ref in ((0, mid), (1, result)):
        for k in range(Z):
            core_copy(u, k).wait_send()
            x_copy(u, k).wait_send()
            final_copy(u, ref, order[k] * Y + mine).wait_send()


def kernel_body(*args):
    n_fs = lax.axis_size("fs")
    Z = n_fs // Y
    hidden, value_p, taps, mgate = args[0], args[2], args[8], args[12]
    rows, width = hidden.shape
    args = list(args)
    for i in (12, 13, 14):
        args[i] = args[i].T
    gap = jnp.zeros((-args[15].shape[0] % ROW,), jnp.float32)
    args[15:17] = [jnp.concatenate([args[15], gap, args[16], gap])]
    blk, ch, hu = width // n_fs, value_p.shape[1], mgate.shape[1]
    args = [a.reshape(1, -1) if a.ndim == 1 else a for a in args]
    lead = -(-(taps.shape[0] - 1) // 8) * 8
    bf16, f32 = jnp.bfloat16, jnp.float32
    dma = pltpu.SemaphoreType.DMA
    n_pieces = 8
    out = pl.pallas_call(
        functools.partial(layer_kernel, Z),
        out_shape=jax.ShapeDtypeStruct((rows, width), bf16),
        in_specs=[
            pl.BlockSpec(memory_space=pl.ANY if i in (0, 12, 13, 14) else pltpu.VMEM)
            for i in range(len(args))
        ],
        out_specs=pl.BlockSpec(memory_space=pl.ANY),
        scratch_shapes=[
            pltpu.VMEM((rows, width), bf16),
            pltpu.VMEM((hu, blk), f32),
            pltpu.VMEM((hu, blk), f32),
            pltpu.VMEM((hu, blk), f32),
            pltpu.VMEM((n_fs, rows, blk), bf16),
            pltpu.VMEM((n_fs, blk, 2 * ch), bf16),
            pltpu.VMEM((n_fs, blk, ch), bf16),
            pltpu.VMEM((n_fs, 2 * hu, blk), bf16),
            pltpu.VMEM((n_fs, hu, blk), bf16),
            pltpu.VMEM((n_fs, rows, blk), bf16),
            pltpu.VMEM((lead + rows, ch), f32),
            pltpu.VMEM((n_fs, rows, blk), bf16),
            pltpu.VMEM((rows, hu), f32),
            pltpu.VMEM((rows, hu), f32),
            pltpu.VMEM((8, rows), f32),
            pltpu.VMEM((3, 8, rows), f32),
            pltpu.VMEM((LANES, rows), f32),
            pltpu.VMEM((2, Z, rows, blk), bf16),
            pltpu.VMEM((2, Z, rows, blk), bf16),
            pltpu.VMEM((2, Z, rows, blk), bf16),
            pltpu.VMEM((2, Z, rows, blk), bf16),
            dma((n_pieces, n_fs, 3)),
            dma((n_pieces, n_fs)),
            dma((3,)),
            dma((3,)),
            dma((2, Z)),
            dma((2, Z)),
            dma((2, Z)),
            dma((2, Z)),
            dma((2, n_fs)),
            dma((2, n_fs)),
            dma((4,)),
            dma((n_fs,)),
        ],
        compiler_params=pltpu.CompilerParams(
            collective_id=0, has_side_effects=True, vmem_limit_bytes=56 * 1024 * 1024
        ),
    )(*args)
    return out


def fits(mesh, args):
    n_fs, n_tp = mesh.shape["fs"], mesh.shape["tp"]
    ch, hu = args[2].shape[1] // n_tp, args[12].shape[1] // n_tp
    blk = args[0].shape[1] // n_fs
    return (
        n_fs % Y == 0
        and n_tp == 2 * CORES
        and ch % LANES == 0
        and hu % 32 == 0
        and blk % (2 * LANES) == 0
        and n_fs <= 8
    )


SPECS = (
    P("fs", None), P(), P("fs", "tp"), P("fs", "tp"), P("fs", "tp"), P("tp"), P("tp"),
    P("fs"), P(None, "tp"), P("tp"), P("tp"), P(), P("fs", "tp"), P("fs", "tp"),
    P("fs", "tp"), P("tp"), P("tp"), P("fs"),
)


def solution(mesh):
    def run(*args):
        return jax.shard_map(
            kernel_body if fits(mesh, args) else body,
            mesh=mesh, in_specs=SPECS, out_specs=P("fs", None), check_vma=False,
        )(*args)

    return run
```

```python
import functools

import jax
import jax.numpy as jnp
from jax import lax
from jax.experimental import pallas as pl
from jax.experimental.pallas import tpu as pltpu
from jax.sharding import PartitionSpec as P


def row_norm(rows, gain):
    scale = lax.rsqrt(jnp.mean(rows * rows, axis=-1, keepdims=True) + 1e-06)
    return rows * scale * gain


def contract_last(left, right):
    return lax.dot_general(
        left, right, (((1,), (1,)), ((), ())), preferred_element_type=jnp.float32
    )


def body(
    hidden_in,
    mix_gain,
    value_proj,
    gate_proj,
    out_proj,
    value_scale,
    gate_scale,
    out_scale,
    conv_kernel,
    norm_gain,
    norm_shift,
    mlp_gain,
    mlp_gate,
    mlp_up,
    mlp_down,
    mlp_gate_scale,
    mlp_up_scale,
    mlp_down_scale,
):
    out_full, down_full = (
        lax.all_gather(out_scale, "fs", axis=0, tiled=True),
        lax.all_gather(mlp_down_scale, "fs", axis=0, tiled=True),
    )
    value_w, gate_w, out_w = (
        lax.all_gather(value_proj.astype(jnp.bfloat16), "fs", axis=0, tiled=True),
        lax.all_gather(gate_proj.astype(jnp.bfloat16), "fs", axis=0, tiled=True),
        lax.all_gather(out_proj.astype(jnp.bfloat16), "fs", axis=0, tiled=True),
    )
    mlp_shards = (
        mlp_gate.astype(jnp.bfloat16),
        mlp_up.astype(jnp.bfloat16),
        mlp_down.astype(jnp.bfloat16),
    )
    rows = hidden_in.astype(jnp.float32)
    normed = row_norm(rows, mix_gain).astype(jnp.bfloat16)
    value_pre = jnp.dot(normed, value_w, preferred_element_type=jnp.float32) * value_scale
    gate_pre = jnp.dot(normed, gate_w, preferred_element_type=jnp.float32) * gate_scale
    glu = value_pre * jax.nn.sigmoid(gate_pre)
    seq_len = glu.shape[0]
    taps = conv_kernel.shape[0]
    padded = jnp.pad(glu, ((taps - 1, 0), (0, 0)))
    kernel = conv_kernel.astype(jnp.float32)
    conved = jnp.zeros_like(glu)
    for tap in range(taps):
        conved = conved + padded[tap : tap + seq_len] * kernel[tap]
    channels = conved.shape[1] * lax.axis_size("tp")
    sums, squares = lax.psum((jnp.sum(conved, axis=1), jnp.sum(conved * conved, axis=1)), "tp")
    chan_mean = (sums / channels)[:, None]
    chan_var = (squares / channels)[:, None] - chan_mean * chan_mean
    act = jax.nn.silu(
        (conved - chan_mean) * lax.rsqrt(chan_var + 1e-05) * norm_gain + norm_shift
    ).astype(jnp.bfloat16)
    conv_term = contract_last(act, out_w) * out_full
    middle_f = (
        (rows + lax.psum(conv_term.astype(jnp.bfloat16), "tp").astype(jnp.float32))
        .astype(jnp.bfloat16)
        .astype(jnp.float32)
    )
    normed_mlp = row_norm(middle_f, mlp_gain).astype(jnp.bfloat16)
    collected = (
        lax.all_gather(mlp_shards[0], "fs", axis=0, tiled=True),
        lax.all_gather(mlp_shards[1], "fs", axis=0, tiled=True),
        lax.all_gather(mlp_shards[2], "fs", axis=0, tiled=True),
    )
    gate_mlp = (
        jnp.dot(normed_mlp, collected[0], preferred_element_type=jnp.float32) * mlp_gate_scale
    )
    up_mlp = jnp.dot(normed_mlp, collected[1], preferred_element_type=jnp.float32) * mlp_up_scale
    hidden_act = (jax.nn.silu(gate_mlp) * up_mlp).astype(jnp.bfloat16)
    mlp_term = contract_last(hidden_act, collected[2]) * down_full
    return (middle_f + lax.psum(mlp_term.astype(jnp.bfloat16), "tp").astype(jnp.float32)).astype(
        jnp.bfloat16
    )


MESH = pl.DeviceIdType.MESH
LANES = 128
Y = 2
CORES = 2
ROW = 1024
AHEAD_Y = 3
AHEAD_Z = 2


def nearest_order(z, extent):
    picks = []
    for k in range(extent):
        pick = jnp.int32(0)
        for at in range(extent):
            order = sorted(range(extent), key=lambda v: (abs(v - at), v))
            pick = jnp.where(z == at, order[k], pick)
        picks.append(pick)
    return picks


def layer_kernel(
    Z,
    hidden_hbm, mix_gain, value_p, gate_p, out_p, value_s, gate_s, out_s, taps_ref,
    norm_gain, norm_shift, mlp_gain, mgate_hbm, mup_hbm, mdown_hbm, mid_s, mdown_s,
    result_hbm,
    hidden, mgate, mup, mdown, result,
    vg, ow, gu, dn, normed, pad, mid, acc, acc_up, stat_out, stat_in, stat_t,
    core_out, core_in, x_out, x_in,
    g_send, g_recv, s_send, s_recv, c_send, c_recv, x_send, x_recv, f_send, f_recv,
    l_sem, o_sem,
):
    f32, bf16 = jnp.float32, jnp.bfloat16
    fs, tp = lax.axis_index("fs"), lax.axis_index("tp")
    z, y = fs // Y, lax.rem(fs, Y)
    x, core = tp // CORES, lax.rem(tp, CORES)
    yo = 1 - y
    me = (fs, tp)
    up, down = (fs + Y, tp), (fs - Y, tp)
    across = (z * Y + yo, tp)
    core_peer = (fs, x * CORES + 1 - core)
    x_peer = (fs, (1 - x) * CORES + core)
    diag_peer = (fs, (1 - x) * CORES + 1 - core)
    has_up, has_down = z < Z - 1, z > 0

    rows, width = hidden.shape
    nblk = Z * Y
    blk = width // nblk
    ch = value_p.shape[1]
    hu = mgate.shape[0]
    fetches = [
        pltpu.make_async_copy(src, dst, l_sem.at[i])
        for i, (src, dst) in enumerate(
            ((hidden_hbm, hidden), (mgate_hbm, mgate), (mup_hbm, mup), (mdown_hbm, mdown))
        )
    ]
    for f in fetches:
        f.start()

    vg[fs, :, :ch] = value_p[...].astype(bf16)
    vg[fs, :, ch:] = gate_p[...].astype(bf16)
    scale_col = jnp.broadcast_to(out_s[...], (LANES, blk)).T
    ow[fs] = (out_p[...].astype(bf16).astype(f32) * scale_col[:, :1]).astype(bf16)

    barrier = pltpu.get_barrier_semaphore()

    def greet(peer):
        pl.semaphore_signal(barrier, inc=1, device_id=peer, device_id_type=MESH)

    for peer in (across, core_peer, x_peer, diag_peer):
        greet(peer)

    @pl.when(has_up)
    def _():
        greet(up)

    @pl.when(has_down)
    def _():
        greet(down)

    pl.semaphore_wait(barrier, 4 + has_up.astype(jnp.int32) + has_down.astype(jnp.int32))

    quarter = hu // 2
    pieces = [(vg, None), (ow, None)]
    pieces += [(gu, (r * quarter, quarter)) for r in range(4)]
    pieces += [(dn, (r * quarter, quarter)) for r in range(2)]
    crossed = (5,)

    def slot(p, at):
        ref, cut = pieces[p]
        return ref.at[at] if cut is None else ref.at[at, pl.ds(*cut)]

    def copy(p, at, peer, way):
        return pltpu.make_async_remote_copy(
            src_ref=slot(p, at), dst_ref=slot(p, at),
            send_sem=g_send.at[p, at, way], recv_sem=g_recv.at[p, at],
            device_id=peer, device_id_type=MESH,
        )

    sent = []

    def start(p, at, peer, way, cond=None):
        if cond is None:
            copy(p, at, peer, way).start()
        else:
            @pl.when(cond)
            def _():
                copy(p, at, peer, way).start()
        sent.append((p, at, peer, way, cond))

    def own_z(p):
        start(p, fs, up, 0, has_up)
        start(p, fs, down, 1, has_down)

    def own_y(p):
        start(p, fs, across, 2)

    def own(p):
        own_y(p)
        own_z(p)

    def arrived(p, at):
        copy(p, at, across, 2).wait_recv()

    def own_crossed(p):
        at = z * Y + yo
        arrived(p, at)
        start(p, at, up, 0, has_up)
        start(p, at, down, 1, has_down)

    def relay(p, s):
        lanes = (y, yo) if p in crossed else (y,)
        for lane in lanes:
            below, above = (z - s) * Y + lane, (z + s) * Y + lane
            ok_b, ok_a = z - s >= 0, z + s < Z

            @pl.when(ok_b)
            def _(below=below):
                arrived(p, below)

            start(p, below, up, 0, jnp.logical_and(ok_b, has_up))
            if p not in crossed:
                start(p, below, across, 2, ok_b)

            @pl.when(ok_a)
            def _(above=above):
                arrived(p, above)

            start(p, above, down, 1, jnp.logical_and(ok_a, has_down))
            if p not in crossed:
                start(p, above, across, 2, ok_a)

    def finish(p, zz=None):
        if p not in crossed:
            for at in range(Z) if zz is None else (zz,):
                arrived(p, at * Y + yo)

    def wave(t):
        q0, count = 2, len(pieces) - 2
        for q in range(AHEAD_Y + 1) if t == 0 else (t + AHEAD_Y,):
            if q < count:
                own_y(q0 + q)
        for q in range(AHEAD_Z + 1) if t == 0 else (t + AHEAD_Z,):
            if q < count:
                own_z(q0 + q)
        if 0 <= t - 1 < count:
            if q0 + t - 1 in crossed:
                own_crossed(q0 + t - 1)
        for s in range(1, Z):
            if 0 <= t - s < count:
                relay(q0 + t - s, s)

    own(0)
    own(1)

    for f in fetches:
        f.wait()
    gu[fs, :hu] = mgate[...].astype(bf16)
    gu[fs, hu:] = mup[...].astype(bf16)
    dn[fs] = (mdown[...].astype(bf16).astype(f32) * mdown_s[...]).astype(bf16)

    relay(0, 1)
    relay(1, 1)

    h = hidden[...].astype(f32)
    norm = lax.rsqrt(jnp.mean(h * h, axis=-1, keepdims=True) + 1e-06)
    for b in range(nblk):
        cols = slice(b * blk, (b + 1) * blk)
        normed[b] = (hidden[:, cols].astype(f32) * norm * mix_gain[:, cols]).astype(bf16)

    for s in range(2, Z):
        relay(0, s)
        relay(1, s)
    wave(0)
    wave(1)
    wave(2)
    finish(0)

    pre = jnp.zeros((rows, 2 * ch), f32)
    for b in range(nblk):
        pre += jnp.dot(normed[b], vg[b], preferred_element_type=f32)
    glu = pre[:, :ch] * value_s[...] * jax.nn.sigmoid(pre[:, ch:] * gate_s[...])
    ntaps = taps_ref.shape[0]
    lead = pad.shape[0] - rows
    pad[pl.ds(0, lead)] = jnp.zeros((lead, ch), f32)
    pad[pl.ds(lead, rows)] = glu
    taps = taps_ref[...].astype(f32)
    conved = jnp.zeros((rows, ch), f32)
    for j in range(ntaps):
        conved += pad[pl.ds(lead - ntaps + 1 + j, rows)] * taps[j : j + 1]
    lane = lax.broadcasted_iota(jnp.int32, (rows, LANES), 1)
    packed = jnp.where(
        lane == 0,
        jnp.sum(conved, axis=1, keepdims=True),
        jnp.sum(conved * conved, axis=1, keepdims=True),
    )
    stat_t[...] = packed.T
    stat_out[...] = stat_t[:8]

    def stat_copy(k, peer):
        return pltpu.make_async_remote_copy(
            src_ref=stat_out, dst_ref=stat_in.at[k],
            send_sem=s_send.at[k], recv_sem=s_recv.at[k],
            device_id=peer, device_id_type=MESH,
        )

    stats = [stat_copy(k, p) for k, p in enumerate((core_peer, x_peer, diag_peer))]
    for c in stats:
        c.start()
    wave(3)
    for c in stats:
        c.wait()
    stat_t[pl.ds(0, 8)] = stat_out[...] + stat_in[0] + stat_in[1] + stat_in[2]
    columns = stat_t[...].T
    channels = ch * CORES * 2
    mean = columns[:, 0:1] / channels
    var = columns[:, 1:2] / channels - mean * mean
    a = (conved - mean) * lax.rsqrt(var + 1e-05) * norm_gain[...] + norm_shift[...]
    act = (a * jax.nn.sigmoid(a)).astype(bf16)
    finish(1)

    order = nearest_order(z, Z)
    mine, theirs = lax.rem(y + core, Y), lax.rem(y + 1 - core, Y)

    def core_copy(u, k):
        return pltpu.make_async_remote_copy(
            src_ref=core_out.at[u, k], dst_ref=core_in.at[u, k],
            send_sem=c_send.at[u, k], recv_sem=c_recv.at[u, k],
            device_id=core_peer, device_id_type=MESH,
        )

    def x_copy(u, k):
        return pltpu.make_async_remote_copy(
            src_ref=x_out.at[u, k], dst_ref=x_in.at[u, k],
            send_sem=x_send.at[u, k], recv_sem=x_recv.at[u, k],
            device_id=x_peer, device_id_type=MESH,
        )

    def final_copy(u, ref, at):
        return pltpu.make_async_remote_copy(
            src_ref=ref.at[at], dst_ref=ref.at[at],
            send_sem=f_send.at[u, at], recv_sem=f_recv.at[u, at],
            device_id=core_peer, device_id_type=MESH,
        )

    def conv_term(b):
        return lax.dot_general(act, ow[b], (((1,), (1,)), ((), ())), preferred_element_type=f32)

    for k in range(Z):
        core_out[0, k] = conv_term(order[k] * Y + theirs).astype(bf16)
        core_copy(0, k).start()
    for k in range(Z):
        term = conv_term(order[k] * Y + mine)
        core_copy(0, k).wait_recv()
        x_out[0, k] = (term + core_in[0, k].astype(f32)).astype(bf16)
        x_copy(0, k).start()
    wave(4)
    for k in range(Z):
        b = order[k] * Y + mine
        x_copy(0, k).wait_recv()
        cols = pl.ds(pl.multiple_of(b * blk, blk), blk)
        total = x_out[0, k].astype(f32) + x_in[0, k].astype(f32)
        mid[b] = (hidden[:, cols].astype(f32) + total).astype(bf16)
        final_copy(0, mid, b).start()
    wave(5)
    for k in range(Z):
        final_copy(0, mid, order[k] * Y + theirs).wait_recv()

    total = jnp.zeros((rows, 1), f32)
    for b in range(nblk):
        m = mid[b].astype(f32)
        total += jnp.sum(m * m, axis=-1, keepdims=True)
    norm = lax.rsqrt(total / width + 1e-06)
    for b in range(nblk):
        cols = slice(b * blk, (b + 1) * blk)
        normed[b] = (mid[b].astype(f32) * norm * mlp_gain[:, cols]).astype(bf16)
    for t in range(6, len(pieces) - 2 + Z - 1):
        wave(t)

    for p in range(2, 6):
        finish(p)
    dims = (((1,), (1,)), ((), ()))

    def gate_up(b):
        return (
            lax.dot_general(normed[b], gu[b, :hu], dims, preferred_element_type=f32),
            lax.dot_general(normed[b], gu[b, hu:], dims, preferred_element_type=f32),
        )

    acc[...], acc_up[...] = gate_up(0)

    def step(b, carry):
        g, u = gate_up(b)
        acc[...] += g
        acc_up[...] += u
        return carry

    lax.fori_loop(1, nblk, step, 0)
    gate = acc[...] * mid_s[:, :hu]
    second = mid_s.shape[1] // 2
    up_v = acc_up[...] * mid_s[:, second : second + hu]
    act2 = (gate * jax.nn.sigmoid(gate) * up_v).astype(bf16)

    def mlp_term(b):
        return jnp.dot(act2, dn[b], preferred_element_type=f32)

    def send_theirs(k):
        core_out[1, k] = mlp_term(order[k] * Y + theirs).astype(bf16)
        core_copy(1, k).start()

    def send_mine(k):
        term = mlp_term(order[k] * Y + mine)
        core_copy(1, k).wait_recv()
        x_out[1, k] = (term + core_in[1, k].astype(f32)).astype(bf16)
        x_copy(1, k).start()

    def send_final(k):
        b = order[k] * Y + mine
        x_copy(1, k).wait_recv()
        total = x_out[1, k].astype(f32) + x_in[1, k].astype(f32)
        result[b] = (mid[b].astype(f32) + total).astype(bf16)
        final_copy(1, result, b).start()
        out_copy(b).start()

    def out_copy(b):
        cols = pl.ds(pl.multiple_of(b * blk, blk), blk)
        return pltpu.make_async_copy(result.at[b], result_hbm.at[:, cols], o_sem.at[b])

    for k in range(Z):
        finish(6, order[k])
        finish(7, order[k])
        send_theirs(k)
        send_mine(k)
        if k:
            send_final(k - 1)
    send_final(Z - 1)
    for k in range(Z):
        b = order[k] * Y + theirs
        final_copy(1, result, b).wait_recv()
        out_copy(b).start()
    for b in range(nblk):
        out_copy(b).wait()

    for p, at, peer, way, cond in sent:
        if cond is None:
            copy(p, at, peer, way).wait_send()
        else:
            @pl.when(cond)
            def _(p=p, at=at, peer=peer, way=way):
                copy(p, at, peer, way).wait_send()
    for u, ref in ((0, mid), (1, result)):
        for k in range(Z):
            core_copy(u, k).wait_send()
            x_copy(u, k).wait_send()
            final_copy(u, ref, order[k] * Y + mine).wait_send()


def kernel_body(*args):
    n_fs = lax.axis_size("fs")
    Z = n_fs // Y
    hidden, value_p, taps, mgate = args[0], args[2], args[8], args[12]
    rows, width = hidden.shape
    args = list(args)
    for i in (12, 13, 14):
        args[i] = args[i].T
    gap = jnp.zeros((-args[15].shape[0] % ROW,), jnp.float32)
    args[15:17] = [jnp.concatenate([args[15], gap, args[16], gap])]
    blk, ch, hu = width // n_fs, value_p.shape[1], mgate.shape[1]
    args = [a.reshape(1, -1) if a.ndim == 1 else a for a in args]
    lead = -(-(taps.shape[0] - 1) // 8) * 8
    bf16, f32 = jnp.bfloat16, jnp.float32
    dma = pltpu.SemaphoreType.DMA
    n_pieces = 8
    out = pl.pallas_call(
        functools.partial(layer_kernel, Z),
        out_shape=jax.ShapeDtypeStruct((rows, width), bf16),
        in_specs=[
            pl.BlockSpec(memory_space=pl.ANY if i in (0, 12, 13, 14) else pltpu.VMEM)
            for i in range(len(args))
        ],
        out_specs=pl.BlockSpec(memory_space=pl.ANY),
        scratch_shapes=[
            pltpu.VMEM((rows, width), bf16),
            pltpu.VMEM((hu, blk), f32),
            pltpu.VMEM((hu, blk), f32),
            pltpu.VMEM((hu, blk), f32),
            pltpu.VMEM((n_fs, rows, blk), bf16),
            pltpu.VMEM((n_fs, blk, 2 * ch), bf16),
            pltpu.VMEM((n_fs, blk, ch), bf16),
            pltpu.VMEM((n_fs, 2 * hu, blk), bf16),
            pltpu.VMEM((n_fs, hu, blk), bf16),
            pltpu.VMEM((n_fs, rows, blk), bf16),
            pltpu.VMEM((lead + rows, ch), f32),
            pltpu.VMEM((n_fs, rows, blk), bf16),
            pltpu.VMEM((rows, hu), f32),
            pltpu.VMEM((rows, hu), f32),
            pltpu.VMEM((8, rows), f32),
            pltpu.VMEM((3, 8, rows), f32),
            pltpu.VMEM((LANES, rows), f32),
            pltpu.VMEM((2, Z, rows, blk), bf16),
            pltpu.VMEM((2, Z, rows, blk), bf16),
            pltpu.VMEM((2, Z, rows, blk), bf16),
            pltpu.VMEM((2, Z, rows, blk), bf16),
            dma((n_pieces, n_fs, 3)),
            dma((n_pieces, n_fs)),
            dma((3,)),
            dma((3,)),
            dma((2, Z)),
            dma((2, Z)),
            dma((2, Z)),
            dma((2, Z)),
            dma((2, n_fs)),
            dma((2, n_fs)),
            dma((4,)),
            dma((n_fs,)),
        ],
        compiler_params=pltpu.CompilerParams(
            collective_id=0, has_side_effects=True, vmem_limit_bytes=56 * 1024 * 1024
        ),
    )(*args)
    return out


def fits(mesh, args):
    n_fs, n_tp = mesh.shape["fs"], mesh.shape["tp"]
    ch, hu = args[2].shape[1] // n_tp, args[12].shape[1] // n_tp
    blk = args[0].shape[1] // n_fs
    return (
        n_fs % Y == 0
        and n_tp == 2 * CORES
        and ch % LANES == 0
        and hu % 32 == 0
        and blk % (2 * LANES) == 0
        and n_fs <= 8
    )


SPECS = (
    P("fs", None), P(), P("fs", "tp"), P("fs", "tp"), P("fs", "tp"), P("tp"), P("tp"),
    P("fs"), P(None, "tp"), P("tp"), P("tp"), P(), P("fs", "tp"), P("fs", "tp"),
    P("fs", "tp"), P("tp"), P("tp"), P("fs"),
)


def solution(mesh):
    def run(*args):
        return jax.shard_map(
            kernel_body if fits(mesh, args) else body,
            mesh=mesh, in_specs=SPECS, out_specs=P("fs", None), check_vma=False,
        )(*args)

    return run
```
